32 devices in a mesh: ep: 8 (over z, x), tp: 4 (over y, core).
Axes of the slice: x: 2, y: 2, z: 4, core: 2. Of those that a mesh axis runs over, the one named last changes fastest.
Arguments:
- tokens: bfloat16 [256, 4096], P('ep'), may hold values from -6 to 6
- routes: int32 [256, 4], P('ep'), may hold values from 0 to 7, all different within a row; in each aligned block of 32 rows (0 to 31, 32 to 63, ...) at most 24 rows name the same one
- mix_weights: float32 [256, 4], P('ep'), may hold values from 0.2 to 1
- pre_gain: float32 [4096], replicated, may hold values from 0.1 to 1.9
- gate_weight: bfloat16 [8, 4096, 2048], P('ep', None, 'tp'), may hold values from -0.09375 to 0.09375
- up_weight: bfloat16 [8, 4096, 2048], P('ep', None, 'tp'), may hold values from -0.09375 to 0.09375
- down_weight: bfloat16 [8, 2048, 4096], P('ep', 'tp'), may hold values from -1 to 1
- post_gain: float32 [4096], P('tp'), may hold values from 0.1 to 1.9
Outputs:
- layer_out: bfloat16 [256, 4096], P('ep', 'tp')
The draws below stay inside these ranges and needn't reach their ends.
Inputs may be any that keep to these rules, and one draw needn't show every extreme that they name: `routes`: within a row the 4 experts differ; among the rows of one index of ep no expert is named more than 24 times.
All inputs are finite; a program needn't handle non-finite values.
Results may differ from the reference program's by a relative error of at most 0.019.
Values may be sent and summed in bfloat16 or wider, within the bound.
A program may use at most 64 MiB of HBM per device.

```python
import math
import jax
import jax.numpy as jnp
import numpy as np
from jax import lax

D = 4096
FF = 2048
TOP = 4
TOK_DEV = 32
EXPERTS = 8
CAP = 24
TOKENS = 256
N_EP = 8
N_TP = 4


def draw_down_weight(key, part):
    noise = jnp.clip(jax.random.normal(jax.random.fold_in(key, 11), (EXPERTS, FF, D), jnp.float32), -6.0, 6.0)
    noise = noise * FF ** (-0.5)
    position = jnp.arange(D, dtype=jnp.float32) / D
    rise = 3.0 ** position * jax.random.uniform(jax.random.fold_in(key, 12), (D,), jnp.float32, 0.6, 1.6)
    return jnp.clip(noise * rise, -1.0, 1.0).astype(jnp.bfloat16)


def steps_of(key, shape, split, smallest, high):
    loudness = 1.0
    for axis_at, parts in split:
        steps = jax.random.uniform(jax.random.fold_in(jax.random.fold_in(key, 6), axis_at), (parts,), jnp.float32, smallest / len(split), high / len(split))
        loudness = loudness * jnp.repeat(jnp.exp(steps), shape[axis_at] // parts).reshape((-1,) + (1,) * (len(shape) - 1 - axis_at))
    return loudness


def assign_block(rng, own, number, rows, amount, top, most, skew):
    order = jax.random.permutation(rng, amount)
    packed, ordinary = portions_of(amount, rows * top, most, skew, True), portions_of(amount, rows * top, most, skew, False)
    places = jnp.arange(amount)

    def named(lengths, offset_by):
        used = int((lengths > 0).sum())
        fixed = max(1, used // 4)
        shifted = fixed + (places - fixed + offset_by * (used - fixed)) % max(1, amount - fixed)
        return jnp.zeros((amount,), jnp.int32).at[order[jnp.where(places < fixed, places, shifted)]].set(jnp.asarray(lengths, jnp.int32))

    lengths = jnp.where(number % 4 == 0, named(packed, number // 4), named(ordinary, number - number // 4 - 1))
    mixed = jax.random.permutation(jax.random.fold_in(own, 3), amount)
    giver, taker = mixed[0:amount // 2 * 2:2], mixed[1:amount // 2 * 2:2]
    margin = jnp.minimum(lengths[giver] - 1, most - lengths[taker]) // 2
    margin = jnp.where((giver == order[0]) | (taker == order[0]) | (lengths[taker] == 0), 0, jnp.maximum(margin, 0))
    shifted = jax.random.randint(jax.random.fold_in(own, 4), (amount // 2,), 0, 1 << 20) % (margin + 1)
    lengths = lengths.at[giver].add(-shifted).at[taker].add(shifted)
    labels = jnp.searchsorted(jnp.cumsum(lengths), jnp.arange(rows * top), side="right").astype(jnp.int32)
    grid = labels.reshape(top, rows).T
    grid = grid[jax.random.permutation(jax.random.fold_in(own, 1), rows)]
    offset_by = jax.random.randint(jax.random.fold_in(own, 2), (rows, 1), 0, top)
    return jnp.take_along_axis(grid, (jnp.arange(top)[None, :] + offset_by) % top, axis=1)


def portions_of(amount, total, limit, lean, full):
    portions = [(1 << 20) // math.isqrt(rank ** lean) + 1 for rank in range(1, amount + 1)]
    largest = limit if full else min(limit, max(-(-total // amount), total * portions[0] // sum(portions)))
    least = 1 if total - largest >= amount - 1 else 0
    given, surplus = [largest] + [least] * (amount - 1), total - largest - least * (amount - 1)
    while surplus > 0:
        free = [i for i in range(1, amount) if given[i] < largest] or [i for i in range(1, amount) if given[i] < limit]
        mass, left = sum([portions[i] for i in free]), surplus
        for i in free:
            extra = min(limit - given[i], max(1, left * portions[i] // mass), surplus)
            given[i] = given[i] + extra
            surplus = surplus - extra
    return np.array(given)


def bell_draw(own_key, extent, deviation, most, split=(), kind=jnp.bfloat16):
    level = steps_of(own_key, extent, split, -0.22, 0.18) if split else 1.0
    values = jax.random.normal(own_key, extent, jnp.float32) * deviation * level
    return jnp.minimum(jnp.maximum(values, -most), most).astype(kind)


def setup_inputs(seed: int = 0) -> dict:
    streams_of = jax.random.split(jax.random.key(seed), 9)
    tokens = bell_draw(streams_of[0], (TOKENS, D), 1.0, 6.0, ((0, 8),))
    routes_keys = jax.random.split(jax.random.fold_in(streams_of[1], 1), TOKENS // TOK_DEV)
    routes_turns = jax.random.permutation(jax.random.fold_in(streams_of[1], 3), TOKENS // TOK_DEV)
    routes = jax.vmap(lambda own, number: assign_block(jax.random.fold_in(streams_of[1], 2), own, number, TOK_DEV, EXPERTS, TOP, CAP, 2))(routes_keys, routes_turns).reshape((TOKENS, TOP))
    mix_weights = jnp.clip(0.2 + 0.8 * jax.random.uniform(streams_of[2], (TOKENS, TOP), jnp.float32) ** steps_of(streams_of[2], (TOKENS, TOP), ((0, 8),), -0.2, 0.2), 0.2, 1.0)
    pre_gain = jnp.clip(1.0 + 0.18 * jax.random.normal(streams_of[3], (D,), jnp.float32), 0.1, 1.9)
    gate_weight = bell_draw(streams_of[4], (EXPERTS, D, FF), D ** -0.5, 0.09375, ((0, 8), (2, 4)))
    up_weight = bell_draw(streams_of[5], (EXPERTS, D, FF), D ** -0.5, 0.09375, ((0, 8), (2, 4)))
    down_weight = draw_down_weight(jax.random.fold_in(streams_of[8], 71), 0)
    post_gain = jnp.clip(1.0 + 0.18 * jax.random.normal(streams_of[7], (D,), jnp.float32), 0.1, 1.9)
    return dict(tokens=tokens, routes=routes, mix_weights=mix_weights, pre_gain=pre_gain, gate_weight=gate_weight, up_weight=up_weight, down_weight=down_weight, post_gain=post_gain)


epsilon = 1e-06

def reference(tokens, routes, mix_weights, pre_gain, gate_weight, up_weight, down_weight, post_gain):
    floats = tokens.astype(jnp.float32)
    normed = (floats * lax.rsqrt(lax.optimization_barrier(jnp.mean(floats * floats, axis=-1, keepdims=True)) + epsilon) * pre_gain).astype(jnp.bfloat16)
    row_slots = N_EP * CAP
    group_width = FF // N_TP

    def visit_expert(result, per_expert):
        w_gate, w_up, w_down, expert_id = per_expert
        matches = routes == expert_id
        weight = lax.optimization_barrier(jnp.sum(jnp.where(matches, mix_weights, 0.0), axis=1))
        is_named = jnp.any(matches, axis=1)
        row_index = jnp.nonzero(is_named, size=row_slots, fill_value=0)[0].astype(jnp.int32)
        is_live = jnp.arange(row_slots) < jnp.sum(is_named.astype(jnp.int32))
        picked = normed[row_index]
        gate_act = jnp.dot(picked, w_gate, preferred_element_type=jnp.float32)
        up_act = jnp.dot(picked, w_up, preferred_element_type=jnp.float32)
        hidden = (jax.nn.silu(gate_act) * up_act).astype(jnp.bfloat16)
        pieces = jnp.einsum('rgf,gfd->grd', hidden.reshape(row_slots, N_TP, group_width).astype(jnp.float32), w_down.reshape(N_TP, group_width, D).astype(jnp.float32))
        pieces = lax.optimization_barrier(pieces.astype(jnp.bfloat16)).astype(jnp.float32)
        expert_out = lax.optimization_barrier(lax.optimization_barrier(jnp.sum(pieces, axis=0)).astype(jnp.bfloat16)).astype(jnp.float32)
        weighting = jnp.where(is_live, weight[row_index], 0.0)
        result = result.at[row_index].add(weighting[:, None] * expert_out)
        return (result, None)
    start = jnp.zeros((tokens.shape[0], D), jnp.float32)
    mixed, _ = lax.scan(visit_expert, start, (gate_weight, up_weight, down_weight, jnp.arange(EXPERTS, dtype=jnp.int32)))
    scale = lax.rsqrt(lax.optimization_barrier(jnp.mean(mixed * mixed, axis=-1, keepdims=True)) + epsilon)
    return (mixed * scale * post_gain).astype(jnp.bfloat16)
```

```python
import functools

import jax
import jax.numpy as jnp
from jax import lax
from jax.experimental import pallas as pl
from jax.experimental.pallas import tpu as pltpu
from jax.sharding import PartitionSpec as P

epsilon = 1e-06
CORES = 2
MESH = pl.DeviceIdType.MESH
VMEM_BYTES = 60 * 1024 * 1024
MAX_COPIES = 256


def fused_kernel(
    S, X, NT,
    tokens, routes, mix, pre_gain, gate_hbm, up_hbm, down_hbm, post_gain, out,
    xg, wg, wu, wd, acc_g, acc_u, hid, wt, wr,
    pown, dsend, drecv, ya, yar, xb, xbr, xa, xar, yb, ybr, keep_a, keep_b,
    za, zar, zb, zbr, st,
    wsem, ssem, gsem, mixs, mixr, dsem, yarsem, xbrsem, xarsem, ybrsem, zarsem, zbrsem, stsem,
):
    R = tokens.shape[0]
    Z, Y = S // X, NT // CORES
    Dq = xg.shape[2]
    H = Dq // 2
    D = tokens.shape[1]
    K = routes.shape[1]
    me, t = lax.axis_index("ep"), lax.axis_index("tp")
    z, x = me // X, lax.rem(me, X)
    y, c = t // CORES, lax.rem(t, CORES)
    pc = 1 - c
    f32, bf16 = jnp.float32, jnp.bfloat16

    def dev(e, q):
        return (e, q)

    def quarter(yy, cc):
        return yy * CORES + cc

    zs = [lax.rem(z + d, Z) for d in range(Z)]
    xs = [lax.rem(x + d, X) for d in range(X)]
    ys = [lax.rem(y + d, Y) for d in range(Y)]
    zm = [lax.rem(z - d + Z, Z) for d in range(Z)]
    xm = [lax.rem(x - d + X, X) for d in range(X)]
    ym = [lax.rem(y - d + Y, Y) for d in range(Y)]

    loads = []
    for i in range(NT):
        for k, (src, dst) in enumerate(((gate_hbm, wg), (up_hbm, wu))):
            loads.append(pltpu.make_async_copy(src.at[0, pl.ds(i * Dq, Dq)], dst.at[i], wsem.at[k, i]))
    for i in range(NT):
        loads.append(pltpu.make_async_copy(down_hbm.at[0, :, pl.ds(i * Dq, Dq)], wd.at[i], wsem.at[2, i]))
    for copy in loads:
        copy.start()

    barrier = pltpu.get_barrier_semaphore()
    for d in range(1, S):
        pl.semaphore_signal(barrier, inc=1, device_id=dev(lax.rem(me + d, S), t), device_id_type=MESH)
    for d in range(1, NT):
        pl.semaphore_signal(barrier, inc=1, device_id=dev(me, lax.rem(t + d, NT)), device_id_type=MESH)

    floats = tokens[...].astype(f32)
    inv = lax.rsqrt(jnp.mean(floats * floats, axis=1, keepdims=True) + epsilon)
    rows = pl.ds(pl.multiple_of(me * R, R), R)
    for q in range(NT):
        cols = slice(q * Dq, (q + 1) * Dq)
        xg[q, rows, :] = (floats[:, cols] * inv * pre_gain[:, cols]).astype(bf16)

    lane = lax.broadcasted_iota(jnp.int32, (R, 128), 1)
    dense = jnp.zeros((R, 128), f32)
    for k in range(K):
        dense = dense + jnp.where(lane == routes[:, k : k + 1], mix[:, k : k + 1], 0.0)
    flipped = jnp.transpose(jnp.concatenate([dense, jnp.zeros((128 - R, 128), f32)], axis=0))
    for e in range(S):
        wt[e] = flipped[e : e + 1, :]
    wr[me] = wt[me]

    pl.semaphore_wait(barrier, S - 1 + NT - 1)

    sends = []

    def send(src, dst, recv_sem, device):
        copy = pltpu.make_async_remote_copy(
            src_ref=src, dst_ref=dst, send_sem=ssem.at[len(sends)], recv_sem=recv_sem,
            device_id=device, device_id_type=MESH,
        )
        copy.start()
        sends.append(copy)

    def arrived(ref, sem):
        pltpu.make_async_remote_copy(
            src_ref=ref, dst_ref=ref, send_sem=ssem.at[0], recv_sem=sem,
            device_id=dev(me, t), device_id_type=MESH,
        ).wait_recv()

    def block(q, s):
        return xg.at[q, pl.ds(pl.multiple_of(s * R, R), R)]

    def send_block(q, s, device):
        send(block(q, s), block(q, s), gsem.at[q, s], device)

    def await_block(q, s):
        arrived(block(q, s), gsem.at[q, s])

    def at(d, dx):
        return zm[d] * X + xm[dx]

    for d in range(1, Z):
        send_block(t, me, dev(zs[d] * X + x, t))
    for dx in range(1, X):
        send_block(t, me, dev(z * X + xs[dx], t))
        for dy in range(1, Y):
            send_block(quarter(ys[dy], c), me, dev(z * X + xs[dx], t))
    for d in range(1, S):
        e = lax.rem(me + d, S)
        send(wt.at[e], wr.at[me], mixr.at[me], dev(e, t))
    for d in range(1, Z):
        s = at(d, 0)
        await_block(t, s)
        for dy in range(1, Y):
            send_block(t, s, dev(me, quarter(ys[dy], c)))
        for dx in range(1, X):
            send_block(t, s, dev(z * X + xs[dx], t))
        send_block(t, s, dev(me, quarter(y, pc)))
    for dx in range(1, X):
        for d in range(Z):
            s = at(d, dx)
            await_block(t, s)
            if d > 0:
                for dy in range(1, Y):
                    send_block(t, s, dev(me, quarter(ys[dy], c)))
            send_block(t, s, dev(me, quarter(y, pc)))
            if d == 0:
                for dy in range(1, Y):
                    await_block(quarter(ys[dy], c), s)
                    send_block(quarter(ys[dy], c), s, dev(me, quarter(y, pc)))

    others = [at(d, dx) for dx in range(X) for d in range(Z) if d or dx]

    def multiply(q, first):
        pltpu.make_async_copy(gate_hbm.at[0, pl.ds(0, Dq)], wg.at[q], wsem.at[0, q]).wait()
        pltpu.make_async_copy(up_hbm.at[0, pl.ds(0, Dq)], wu.at[q], wsem.at[1, q]).wait()
        for w, acc in ((wg, acc_g), (wu, acc_u)):
            part = jnp.dot(xg[q], w[q], preferred_element_type=f32)
            acc[...] = part if first else acc[...] + part

    multiply(t, True)
    for s in others:
        await_block(quarter(y, pc), s)
    multiply(quarter(y, pc), False)
    for dy in range(1, Y):
        for dx in range(X):
            for d in range(1, Z):
                s = at(d, dx)
                await_block(quarter(ym[dy], c), s)
                send_block(quarter(ym[dy], c), s, dev(me, quarter(y, pc)))
        multiply(quarter(ym[dy], c), False)
    for dy in range(1, Y):
        for s in others:
            await_block(quarter(ym[dy], pc), s)
        multiply(quarter(ym[dy], pc), False)

    for d in range(1, S):
        s = lax.rem(me + d, S)
        arrived(wr.at[s], mixr.at[s])
    named = jnp.concatenate([wr[s] for s in range(S)] + [jnp.zeros((128 - S, 128), f32)], axis=0)
    columns = jnp.transpose(named)
    weight = jnp.concatenate([columns[:R, s : s + 1] for s in range(S)], axis=0)
    gate = acc_g[...]
    hid[...] = (gate / (1.0 + jnp.exp(-gate)) * acc_u[...] * weight).astype(bf16)

    def down(q):
        pltpu.make_async_copy(down_hbm.at[0, :, pl.ds(0, Dq)], wd.at[q], wsem.at[2, q]).wait()
        return jnp.dot(hid[...], wd[q], preferred_element_type=f32)

    y_order = [ys[dy] for dy in range(1, Y)] + [y]
    for yy in y_order:
        part = down(quarter(yy, pc)).astype(bf16)
        for h in range(2):
            for s in range(S):
                dsend[yy, h, s // X, s % X] = part[s * R : (s + 1) * R, h * H : (h + 1) * H]
            send(dsend.at[yy, h], drecv.at[yy, h], dsem.at[yy, h], dev(me, quarter(y, pc)))
    for yy in y_order:
        part = down(quarter(yy, c))
        for h in range(2):
            for s in range(S):
                pown[yy, h, s // X, s % X] = part[s * R : (s + 1) * R, h * H : (h + 1) * H]

    def own(yy, h, j, xx):
        return pown[yy, h, j, xx] + drecv[yy, h, j, xx].astype(f32)

    js = [zs[d] for d in range(1, Z)] + [z]
    for yy in y_order:
        for h in range(2):
            arrived(drecv.at[yy, h], dsem.at[yy, h])
    for j in js:
        for dy in range(1, Y):
            for xx in range(X):
                ya[dy, j, xx] = own(ys[dy], 0, j, xx).astype(bf16)
            send(ya.at[dy, j], yar.at[dy, j], yarsem.at[dy, j], dev(me, quarter(ys[dy], c)))
        for dx in range(1, X):
            for yy in y_order:
                xb[dx, yy, j] = own(yy, 1, j, xs[dx]).astype(bf16)
                send(xb.at[dx, yy, j], xbr.at[dx, yy, j], xbrsem.at[dx, yy, j], dev(z * X + xs[dx], t))
    for j in js:
        for yy in y_order:
            total = own(yy, 1, j, x)
            for dx in range(1, X):
                arrived(xbr.at[dx, yy, j], xbrsem.at[dx, yy, j])
                total = total + xbr[dx, yy, j].astype(f32)
            keep_b[yy, j] = total
        for dy in range(1, Y):
            yb[dy, j] = keep_b[ys[dy], j].astype(bf16)
            send(yb.at[dy, j], ybr.at[dy, j], ybrsem.at[dy, j], dev(me, quarter(ys[dy], c)))
        for dy in range(1, Y):
            arrived(yar.at[dy, j], yarsem.at[dy, j])
        for dx in list(range(1, X)) + [0]:
            total = own(y, 0, j, xs[dx])
            for dy in range(1, Y):
                total = total + yar[dy, j, xs[dx]].astype(f32)
            if dx == 0:
                keep_a[j] = total
            else:
                xa[dx, j] = total.astype(bf16)
                send(xa.at[dx, j], xar.at[dx, j], xarsem.at[dx, j], dev(z * X + xs[dx], t))
    for at_d, j in enumerate(js):
        d = (at_d + 1) % Z
        total_a = keep_a[j]
        for dx in range(1, X):
            arrived(xar.at[dx, j], xarsem.at[dx, j])
            total_a = total_a + xar[dx, j].astype(f32)
        if d:
            za[d] = total_a.astype(bf16)
            send(za.at[d], zar.at[d], zarsem.at[d], dev(j * X + x, t))
        total_b = keep_b[y, j]
        for dy in range(1, Y):
            arrived(ybr.at[dy, j], ybrsem.at[dy, j])
            total_b = total_b + ybr[dy, j].astype(f32)
        if d:
            zb[d] = total_b.astype(bf16)
            send(zb.at[d], zbr.at[d], zbrsem.at[d], dev(j * X + x, t))
    for d in range(1, Z):
        arrived(zar.at[d], zarsem.at[d])
        total_a = total_a + zar[d].astype(f32)
        arrived(zbr.at[d], zbrsem.at[d])
        total_b = total_b + zbr[d].astype(f32)

    squares = jnp.sum(total_a * total_a, axis=1, keepdims=True) + jnp.sum(
        total_b * total_b, axis=1, keepdims=True
    )
    st[0] = jnp.broadcast_to(squares, (R, 128))
    for d in range(1, NT):
        send(st.at[0], st.at[d], stsem.at[d], dev(me, lax.rem(t + d, NT)))
    for d in range(1, NT):
        arrived(st.at[d], stsem.at[d])
        squares = squares + st[d][:, 0:1]
    scale = lax.rsqrt(squares / D + epsilon)
    out[:, 0:H] = (total_a * scale * post_gain[:, 0:H]).astype(bf16)
    out[:, H:Dq] = (total_b * scale * post_gain[:, H:Dq]).astype(bf16)
    for copy in sends:
        copy.wait_send()


def fused(S, X, NT, tokens, routes, mix_weights, pre_gain, gate_weight, up_weight, down_weight, post_gain):
    R, D = tokens.shape
    F = gate_weight.shape[2]
    Dq = D // NT
    H = Dq // 2
    Z, Y = S // X, NT // CORES
    f32, bf16 = jnp.float32, jnp.bfloat16
    dma, vmem = pltpu.SemaphoreType.DMA, pltpu.VMEM
    in_vmem, anywhere = pl.BlockSpec(memory_space=pltpu.VMEM), pl.BlockSpec(memory_space=pl.ANY)
    return pl.pallas_call(
        functools.partial(fused_kernel, S, X, NT),
        out_shape=jax.ShapeDtypeStruct((R, Dq), bf16),
        in_specs=[in_vmem] * 4 + [anywhere] * 3 + [in_vmem],
        out_specs=in_vmem,
        scratch_shapes=[
            vmem((NT, S * R, Dq), bf16),
            vmem((NT, Dq, F), bf16),
            vmem((NT, Dq, F), bf16),
            vmem((NT, F, Dq), bf16),
            vmem((S * R, F), f32),
            vmem((S * R, F), f32),
            vmem((S * R, F), bf16),
            vmem((S, 1, 128), f32),
            vmem((S, 1, 128), f32),
            vmem((Y, 2, Z, X, R, H), f32),
            vmem((Y, 2, Z, X, R, H), bf16),
            vmem((Y, 2, Z, X, R, H), bf16),
            vmem((Y, Z, X, R, H), bf16),
            vmem((Y, Z, X, R, H), bf16),
            vmem((X, Y, Z, R, H), bf16),
            vmem((X, Y, Z, R, H), bf16),
            vmem((X, Z, R, H), bf16),
            vmem((X, Z, R, H), bf16),
            vmem((Y, Z, R, H), bf16),
            vmem((Y, Z, R, H), bf16),
            vmem((Z, R, H), f32),
            vmem((Y, Z, R, H), f32),
            vmem((Z, R, H), bf16),
            vmem((Z, R, H), bf16),
            vmem((Z, R, H), bf16),
            vmem((Z, R, H), bf16),
            vmem((NT, R, 128), f32),
            dma((3, NT)),
            dma((MAX_COPIES,)),
            dma((NT, S)),
            dma((S,)),
            dma((S,)),
            dma((Y, 2)),
            dma((Y, Z)),
            dma((X, Y, Z)),
            dma((X, Z)),
            dma((Y, Z)),
            dma((Z,)),
            dma((Z,)),
            dma((NT,)),
        ],
        compiler_params=pltpu.CompilerParams(
            collective_id=0, has_side_effects=True, vmem_limit_bytes=VMEM_BYTES
        ),
    )(
        tokens, routes, mix_weights, pre_gain.reshape(1, D), gate_weight, up_weight, down_weight,
        post_gain.reshape(1, Dq),
    )


def routed(
    tokens, routes, mix_weights, pre_gain, gate_weight, up_weight, down_weight, post_gain
):
    tok_rows, width = tokens.shape
    top_count = routes.shape[1]
    experts = lax.axis_size("ep")
    capacity = min(tok_rows, max(2, (3 * tok_rows * top_count + 2 * experts - 1) // (2 * experts)))
    floats = tokens.astype(jnp.float32)
    normed = (
        floats * lax.rsqrt(jnp.mean(floats * floats, axis=-1, keepdims=True) + epsilon) * pre_gain
    ).astype(jnp.bfloat16)
    chosen = routes.reshape(-1)
    onehot = (chosen[:, None] == jnp.arange(experts, dtype=jnp.int32)[None, :]).astype(jnp.int32)
    before = jnp.cumsum(onehot, axis=0) - onehot
    slot_rank = jnp.sum(before * onehot, axis=1)
    target = chosen * capacity + slot_rank
    placed = target[:, None] == jnp.arange(experts * capacity, dtype=jnp.int32)[None, :]
    by_choice = placed.reshape(tok_rows, top_count, experts * capacity)
    picked = jnp.any(by_choice, axis=1).astype(jnp.bfloat16)
    outgoing = jnp.einsum("tc,td->cd", picked, normed, preferred_element_type=jnp.float32).astype(
        jnp.bfloat16
    )
    outgoing = outgoing.reshape(experts, capacity, width)
    slice_width = width // lax.axis_size("tp")
    outgoing_part = lax.dynamic_slice_in_dim(
        outgoing, lax.axis_index("tp") * slice_width, slice_width, 2
    )
    arrived = lax.all_to_all(outgoing_part, "ep", split_axis=0, concat_axis=0, tiled=True)
    arrived = lax.all_gather(arrived, "tp", axis=2, tiled=True)
    arrived_rows = arrived.reshape(experts * capacity, width)
    gate_act = jnp.dot(arrived_rows, gate_weight[0], preferred_element_type=jnp.float32)
    up_act = jnp.dot(arrived_rows, up_weight[0], preferred_element_type=jnp.float32)
    hidden = (jax.nn.silu(gate_act) * up_act).astype(jnp.bfloat16)
    partial_value = jnp.dot(hidden, down_weight[0], preferred_element_type=jnp.float32)
    summed = lax.psum_scatter(
        partial_value.astype(jnp.bfloat16), "tp", scatter_dimension=1, tiled=True
    )
    returned = lax.all_to_all(
        summed.reshape(experts, capacity, summed.shape[1]),
        "ep",
        split_axis=0,
        concat_axis=0,
        tiled=True,
    )
    results = returned.reshape(experts * capacity, summed.shape[1]).astype(jnp.float32)
    mixing = jnp.sum(mix_weights[:, :, None] * by_choice.astype(jnp.float32), axis=1)
    mixed = jnp.dot(mixing, results, precision=lax.Precision.HIGHEST)
    squares = jnp.sum(mixed * mixed, axis=1)
    total = lax.psum(squares, "tp")
    scale = lax.rsqrt(total / width + epsilon)
    return (mixed * scale[:, None] * post_gain).astype(jnp.bfloat16)


def copies_of(S, X, NT):
    Z, Y = S // X, NT // CORES
    gather = Z - 1 + (X - 1) * Y + S - 1 + NT * S * 2 * X
    back = 2 * Y + Z * (Y - 1 + (X - 1) * Y + Y - 1 + X - 1) + 2 * Z + NT
    return gather + back


def solution(mesh):
    in_specs = (
        P("ep", None),
        P("ep", None),
        P("ep", None),
        P(),
        P("ep", None, "tp"),
        P("ep", None, "tp"),
        P("ep", "tp", None),
        P("tp"),
    )
    out_specs = P("ep", "tp")
    S, NT = mesh.shape["ep"], mesh.shape["tp"]
    X = 2
    on_device = routed
    if S % X == 0 and NT % CORES == 0 and copies_of(S, X, NT) <= MAX_COPIES:
        on_device = functools.partial(fused, S, X, NT)
    return jax.shard_map(
        on_device, mesh=mesh, in_specs=in_specs, out_specs=out_specs, check_vma=False
    )
```

```python
import functools

import jax
import jax.numpy as jnp
from jax import lax
from jax.experimental import pallas as pl
from jax.experimental.pallas import tpu as pltpu
from jax.sharding import PartitionSpec as P

epsilon = 1e-06
CORES = 2
MESH = pl.DeviceIdType.MESH
VMEM_BYTES = 60 * 1024 * 1024
MAX_COPIES = 512
SUB = 2


def fused_kernel(
    S, X, NT,
    tokens, routes, mix, pre_gain, gate_hbm, up_hbm, down_hbm, post_gain, out,
    xg, wg, wu, wd, acc_g, acc_u, hid, wt, wr,
    pown, dsend, drecv, ya, yar, xb, xbr, xa, xar, yb, ybr, keep_a, keep_b,
    za, zar, zb, zbr, st,
    wsem, ssem, gsem, mixr, dsem, yarsem, xbrsem, xarsem, ybrsem, zarsem, zbrsem, stsem,
):
    R = tokens.shape[0]
    Z, Y = S // X, NT // CORES
    Dq = xg.shape[2]
    W = 2 * SUB
    H = Dq // W
    D = tokens.shape[1]
    K = routes.shape[0]
    R2 = R // SUB
    me, t = lax.axis_index("ep"), lax.axis_index("tp")
    z, x = me // X, lax.rem(me, X)
    y, c = t // CORES, lax.rem(t, CORES)
    pc = 1 - c
    f32, bf16 = jnp.float32, jnp.bfloat16

    def dev(e, q):
        return (e, q)

    def quarter(yy, cc):
        return yy * CORES + cc

    def flip(v, m):
        for b in range(m.bit_length()):
            if m >> b & 1:
                v = v + (1 << b) * (1 - 2 * lax.rem(v // (1 << b), 2))
        return v

    if Z & (Z - 1) == 0:
        zs = [z] + [flip(z, m) for m in range(Z - 1, 0, -1)]
        zm = zs
    else:
        zs = [lax.rem(z + d, Z) for d in range(Z)]
        zm = [lax.rem(z - d + Z, Z) for d in range(Z)]
    xs = [lax.rem(x + d, X) for d in range(X)]
    ys = [lax.rem(y + d, Y) for d in range(Y)]
    xm = [lax.rem(x - d + X, X) for d in range(X)]
    ym = [lax.rem(y - d + Y, Y) for d in range(Y)]

    loads = []
    for i in range(NT):
        for k, (src, dst) in enumerate(((gate_hbm, wg), (up_hbm, wu))):
            loads.append(pltpu.make_async_copy(src.at[0, pl.ds(i * Dq, Dq)], dst.at[i], wsem.at[k, i]))
    for i in range(NT):
        loads.append(pltpu.make_async_copy(down_hbm.at[0, :, pl.ds(i * Dq, Dq)], wd.at[i], wsem.at[2, i]))
    for copy in loads:
        copy.start()

    barrier = pltpu.get_barrier_semaphore()
    for d in range(1, S):
        pl.semaphore_signal(barrier, inc=1, device_id=dev(lax.rem(me + d, S), t), device_id_type=MESH)
    for d in range(1, NT):
        pl.semaphore_signal(barrier, inc=1, device_id=dev(me, lax.rem(t + d, NT)), device_id_type=MESH)

    floats = tokens[...].astype(f32)
    inv = lax.rsqrt(jnp.mean(floats * floats, axis=1, keepdims=True) + epsilon)
    rows = pl.ds(pl.multiple_of(me * R, R), R)
    for q in range(NT):
        cols = slice(q * Dq, (q + 1) * Dq)
        xg[q, rows, :] = (floats[:, cols] * inv * pre_gain[:, cols]).astype(bf16)

    for e in range(S):
        dense = jnp.zeros((1, R), f32)
        for k in range(K):
            dense = dense + jnp.where(routes[k : k + 1, :] == e, mix[k : k + 1, :], 0.0)
        wt[e] = jnp.concatenate([dense, jnp.zeros((1, 128 - R), f32)], axis=1)
    wr[me] = wt[me]

    pl.semaphore_wait(barrier, S - 1 + NT - 1)

    sends = []

    def send(src, dst, recv_sem, device):
        copy = pltpu.make_async_remote_copy(
            src_ref=src, dst_ref=dst, send_sem=ssem.at[len(sends)], recv_sem=recv_sem,
            device_id=device, device_id_type=MESH,
        )
        copy.start()
        sends.append(copy)

    def arrived(ref, sem):
        pltpu.make_async_remote_copy(
            src_ref=ref, dst_ref=ref, send_sem=ssem.at[0], recv_sem=sem,
            device_id=dev(me, t), device_id_type=MESH,
        ).wait_recv()

    def block(q, s, i):
        return xg.at[q, pl.ds(pl.multiple_of(s * R + i * R2, R2), R2)]

    def send_block(q, s, i, device):
        send(block(q, s, i), block(q, s, i), gsem.at[q, s, i], device)

    def await_block(q, s):
        for i in range(SUB):
            arrived(block(q, s, i), gsem.at[q, s, i])

    def await_part(q, s, i):
        arrived(block(q, s, i), gsem.at[q, s, i])

    def at(d, dx):
        return zm[d] * X + xm[dx]

    for d in range(1, Z):
        for i in range(SUB):
            send_block(t, me, i, dev(zs[d] * X + x, t))
    for dx in range(1, X):
        for i in range(SUB):
            send_block(t, me, i, dev(z * X + xs[dx], t))
            for dy in range(1, Y):
                send_block(quarter(ys[dy], c), me, i, dev(z * X + xs[dx], t))
    for d in range(1, S):
        e = lax.rem(me + d, S)
        send(wt.at[e], wr.at[me], mixr.at[me], dev(e, t))
    for d in range(1, Z):
        s = at(d, 0)
        for i in range(SUB):
            await_part(t, s, i)
            for dx in range(1, X):
                send_block(t, s, i, dev(z * X + xs[dx], t))
            for dy in range(1, Y):
                send_block(t, s, i, dev(me, quarter(ys[dy], c)))
            send_block(t, s, i, dev(me, quarter(y, pc)))
    for dx in range(1, X):
        for d in range(Z):
            s = at(d, dx)
            for i in range(SUB):
                await_part(t, s, i)
                if d > 0:
                    for dy in range(1, Y):
                        send_block(t, s, i, dev(me, quarter(ys[dy], c)))
                send_block(t, s, i, dev(me, quarter(y, pc)))
                if d == 0:
                    for dy in range(1, Y):
                        await_part(quarter(ys[dy], c), s, i)
                        send_block(quarter(ys[dy], c), s, i, dev(me, quarter(y, pc)))

    others = [at(d, dx) for dx in range(X) for d in range(Z) if d or dx]

    def multiply(q, first):
        pltpu.make_async_copy(gate_hbm.at[0, pl.ds(0, Dq)], wg.at[q], wsem.at[0, q]).wait()
        pltpu.make_async_copy(up_hbm.at[0, pl.ds(0, Dq)], wu.at[q], wsem.at[1, q]).wait()
        for w, acc in ((wg, acc_g), (wu, acc_u)):
            part = jnp.dot(xg[q], w[q], preferred_element_type=f32)
            acc[...] = part if first else acc[...] + part

    multiply(t, True)
    for s in others:
        await_block(quarter(y, pc), s)
    multiply(quarter(y, pc), False)
    for dy in range(1, Y):
        for dx in range(X):
            for d in range(1, Z):
                s = at(d, dx)
                for i in range(SUB):
                    await_part(quarter(ym[dy], c), s, i)
                    send_block(quarter(ym[dy], c), s, i, dev(me, quarter(y, pc)))
        multiply(quarter(ym[dy], c), False)
    for dy in range(1, Y):
        for s in others:
            await_block(quarter(ym[dy], pc), s)
        multiply(quarter(ym[dy], pc), False)

    for d in range(1, S):
        s = lax.rem(me + d, S)
        arrived(wr.at[s], mixr.at[s])
    named = jnp.concatenate([wr[s] for s in range(S)] + [jnp.zeros((128 - S, 128), f32)], axis=0)
    columns = jnp.transpose(named)
    weight = jnp.concatenate([columns[:R, s : s + 1] for s in range(S)], axis=0)
    gate = acc_g[...]
    hid[...] = (gate / (1.0 + jnp.exp(-gate)) * acc_u[...] * weight).astype(bf16)

    def down(q):
        pltpu.make_async_copy(down_hbm.at[0, :, pl.ds(0, Dq)], wd.at[q], wsem.at[2, q]).wait()
        return jnp.dot(hid[...], wd[q], preferred_element_type=f32)

    y_order = [ys[dy] for dy in range(1, Y)] + [y]
    js = [zs[d] for d in range(1, Z)] + [z]
    first, second = list(range(SUB)), list(range(SUB, W))

    def own(yy, h, j, xx):
        return pown[yy, h, j, xx] + drecv[yy, h, j, xx].astype(f32)

    def await_core(yy, h):
        arrived(drecv.at[yy, h], dsem.at[yy, h])

    for yy in y_order:
        part = down(quarter(yy, pc)).astype(bf16)
        for h in second + first if yy is y else first + second:
            for s in range(S):
                dsend[yy, h, s // X, s % X] = part[s * R : (s + 1) * R, h * H : (h + 1) * H]
            send(dsend.at[yy, h], drecv.at[yy, h], dsem.at[yy, h], dev(me, quarter(y, pc)))
    for dy in list(range(1, Y)) + [0]:
        yy = ys[dy]
        part = down(quarter(yy, c))
        for h in range(W):
            for s in range(S):
                pown[yy, h, s // X, s % X] = part[s * R : (s + 1) * R, h * H : (h + 1) * H]
        if dy:
            for h in first:
                await_core(yy, h)
            for j in js:
                for h in first:
                    for xx in range(X):
                        ya[dy, h, j, xx] = own(yy, h, j, xx).astype(bf16)
                    send(ya.at[dy, h, j], yar.at[dy, h, j], yarsem.at[dy, h, j], dev(me, quarter(yy, c)))
        for h in second:
            await_core(yy, h)
        for j in js:
            for h in second:
                for dx in range(1, X):
                    xb[dx, yy, h - SUB, j] = own(yy, h, j, xs[dx]).astype(bf16)
                    send(
                        xb.at[dx, yy, h - SUB, j], xbr.at[dx, yy, h - SUB, j],
                        xbrsem.at[dx, yy, h - SUB, j], dev(z * X + xs[dx], t),
                    )
    for h in first:
        await_core(y, h)
    for j in js:
        for i in range(SUB):
            for yy in y_order:
                total = own(yy, SUB + i, j, x)
                for dx in range(1, X):
                    arrived(xbr.at[dx, yy, i, j], xbrsem.at[dx, yy, i, j])
                    total = total + xbr[dx, yy, i, j].astype(f32)
                keep_b[yy, i, j] = total
            for dy in range(1, Y):
                yb[dy, i, j] = keep_b[ys[dy], i, j].astype(bf16)
                send(yb.at[dy, i, j], ybr.at[dy, i, j], ybrsem.at[dy, i, j], dev(me, quarter(ys[dy], c)))
            for dy in range(1, Y):
                arrived(yar.at[dy, i, j], yarsem.at[dy, i, j])
            for dx in list(range(1, X)) + [0]:
                total = own(y, i, j, xs[dx])
                for dy in range(1, Y):
                    total = total + yar[dy, i, j, xs[dx]].astype(f32)
                if dx == 0:
                    keep_a[i, j] = total
                else:
                    xa[dx, i, j] = total.astype(bf16)
                    send(xa.at[dx, i, j], xar.at[dx, i, j], xarsem.at[dx, i, j], dev(z * X + xs[dx], t))
    mine = {}
    for at_d, j in enumerate(js):
        d = (at_d + 1) % Z
        for i in range(SUB):
            total = keep_a[i, j]
            for dx in range(1, X):
                arrived(xar.at[dx, i, j], xarsem.at[dx, i, j])
                total = total + xar[dx, i, j].astype(f32)
            if d:
                za[d, i] = total.astype(bf16)
                send(za.at[d, i], zar.at[d, i], zarsem.at[d, i], dev(j * X + x, t))
            else:
                mine[i] = total
            total = keep_b[y, i, j]
            for dy in range(1, Y):
                arrived(ybr.at[dy, i, j], ybrsem.at[dy, i, j])
                total = total + ybr[dy, i, j].astype(f32)
            if d:
                zb[d, i] = total.astype(bf16)
                send(zb.at[d, i], zbr.at[d, i], zbrsem.at[d, i], dev(j * X + x, t))
            else:
                mine[SUB + i] = total
    for d in range(1, Z):
        for i in range(SUB):
            arrived(zar.at[d, i], zarsem.at[d, i])
            mine[i] = mine[i] + zar[d, i].astype(f32)
            arrived(zbr.at[d, i], zbrsem.at[d, i])
            mine[SUB + i] = mine[SUB + i] + zbr[d, i].astype(f32)

    squares = jnp.zeros((R, 1), f32)
    for h in range(W):
        squares = squares + jnp.sum(mine[h] * mine[h], axis=1, keepdims=True)
    st[0] = jnp.broadcast_to(squares, (R, 128))
    for d in range(1, NT):
        send(st.at[0], st.at[d], stsem.at[d], dev(me, lax.rem(t + d, NT)))
    for d in range(1, NT):
        arrived(st.at[d], stsem.at[d])
        squares = squares + st[d][:, 0:1]
    scale = lax.rsqrt(squares / D + epsilon)
    for h in range(W):
        cols = slice(h * H, (h + 1) * H)
        out[:, cols] = (mine[h] * scale * post_gain[:, cols]).astype(bf16)
    for copy in sends:
        copy.wait_send()


def fused(S, X, NT, tokens, routes, mix_weights, pre_gain, gate_weight, up_weight, down_weight, post_gain):
    R, D = tokens.shape
    F = gate_weight.shape[2]
    Dq = D // NT
    W = 2 * SUB
    H = Dq // W
    Z, Y = S // X, NT // CORES
    f32, bf16 = jnp.float32, jnp.bfloat16
    dma, vmem = pltpu.SemaphoreType.DMA, pltpu.VMEM
    in_vmem, anywhere = pl.BlockSpec(memory_space=pltpu.VMEM), pl.BlockSpec(memory_space=pl.ANY)
    return pl.pallas_call(
        functools.partial(fused_kernel, S, X, NT),
        out_shape=jax.ShapeDtypeStruct((R, Dq), bf16),
        in_specs=[in_vmem] * 4 + [anywhere] * 3 + [in_vmem],
        out_specs=in_vmem,
        scratch_shapes=[
            vmem((NT, S * R, Dq), bf16),
            vmem((NT, Dq, F), bf16),
            vmem((NT, Dq, F), bf16),
            vmem((NT, F, Dq), bf16),
            vmem((S * R, F), f32),
            vmem((S * R, F), f32),
            vmem((S * R, F), bf16),
            vmem((S, 1, 128), f32),
            vmem((S, 1, 128), f32),
            vmem((Y, W, Z, X, R, H), f32),
            vmem((Y, W, Z, X, R, H), bf16),
            vmem((Y, W, Z, X, R, H), bf16),
            vmem((Y, SUB, Z, X, R, H), bf16),
            vmem((Y, SUB, Z, X, R, H), bf16),
            vmem((X, Y, SUB, Z, R, H), bf16),
            vmem((X, Y, SUB, Z, R, H), bf16),
            vmem((X, SUB, Z, R, H), bf16),
            vmem((X, SUB, Z, R, H), bf16),
            vmem((Y, SUB, Z, R, H), bf16),
            vmem((Y, SUB, Z, R, H), bf16),
            vmem((SUB, Z, R, H), f32),
            vmem((Y, SUB, Z, R, H), f32),
            vmem((Z, SUB, R, H), bf16),
            vmem((Z, SUB, R, H), bf16),
            vmem((Z, SUB, R, H), bf16),
            vmem((Z, SUB, R, H), bf16),
            vmem((NT, R, 128), f32),
            dma((3, NT)),
            dma((copies_of(S, X, NT),)),
            dma((NT, S, SUB)),
            dma((S,)),
            dma((Y, W)),
            dma((Y, SUB, Z)),
            dma((X, Y, SUB, Z)),
            dma((X, SUB, Z)),
            dma((Y, SUB, Z)),
            dma((Z, SUB)),
            dma((Z, SUB)),
            dma((NT,)),
        ],
        compiler_params=pltpu.CompilerParams(
            collective_id=0, has_side_effects=True, vmem_limit_bytes=VMEM_BYTES
        ),
    )(
        tokens, routes.T, mix_weights.T, pre_gain.reshape(1, D), gate_weight, up_weight, down_weight,
        post_gain.reshape(1, Dq),
    )


def routed(
    tokens, routes, mix_weights, pre_gain, gate_weight, up_weight, down_weight, post_gain
):
    tok_rows, width = tokens.shape
    top_count = routes.shape[1]
    experts = lax.axis_size("ep")
    capacity = min(tok_rows, max(2, (3 * tok_rows * top_count + 2 * experts - 1) // (2 * experts)))
    floats = tokens.astype(jnp.float32)
    normed = (
        floats * lax.rsqrt(jnp.mean(floats * floats, axis=-1, keepdims=True) + epsilon) * pre_gain
    ).astype(jnp.bfloat16)
    chosen = routes.reshape(-1)
    onehot = (chosen[:, None] == jnp.arange(experts, dtype=jnp.int32)[None, :]).astype(jnp.int32)
    before = jnp.cumsum(onehot, axis=0) - onehot
    slot_rank = jnp.sum(before * onehot, axis=1)
    target = chosen * capacity + slot_rank
    placed = target[:, None] == jnp.arange(experts * capacity, dtype=jnp.int32)[None, :]
    by_choice = placed.reshape(tok_rows, top_count, experts * capacity)
    picked = jnp.any(by_choice, axis=1).astype(jnp.bfloat16)
    outgoing = jnp.einsum("tc,td->cd", picked, normed, preferred_element_type=jnp.float32).astype(
        jnp.bfloat16
    )
    outgoing = outgoing.reshape(experts, capacity, width)
    slice_width = width // lax.axis_size("tp")
    outgoing_part = lax.dynamic_slice_in_dim(
        outgoing, lax.axis_index("tp") * slice_width, slice_width, 2
    )
    arrived = lax.all_to_all(outgoing_part, "ep", split_axis=0, concat_axis=0, tiled=True)
    arrived = lax.all_gather(arrived, "tp", axis=2, tiled=True)
    arrived_rows = arrived.reshape(experts * capacity, width)
    gate_act = jnp.dot(arrived_rows, gate_weight[0], preferred_element_type=jnp.float32)
    up_act = jnp.dot(arrived_rows, up_weight[0], preferred_element_type=jnp.float32)
    hidden = (jax.nn.silu(gate_act) * up_act).astype(jnp.bfloat16)
    partial_value = jnp.dot(hidden, down_weight[0], preferred_element_type=jnp.float32)
    summed = lax.psum_scatter(
        partial_value.astype(jnp.bfloat16), "tp", scatter_dimension=1, tiled=True
    )
    returned = lax.all_to_all(
        summed.reshape(experts, capacity, summed.shape[1]),
        "ep",
        split_axis=0,
        concat_axis=0,
        tiled=True,
    )
    results = returned.reshape(experts * capacity, summed.shape[1]).astype(jnp.float32)
    mixing = jnp.sum(mix_weights[:, :, None] * by_choice.astype(jnp.float32), axis=1)
    mixed = jnp.dot(mixing, results, precision=lax.Precision.HIGHEST)
    squares = jnp.sum(mixed * mixed, axis=1)
    total = lax.psum(squares, "tp")
    scale = lax.rsqrt(total / width + epsilon)
    return (mixed * scale[:, None] * post_gain).astype(jnp.bfloat16)


def copies_of(S, X, NT):
    Z, Y = S // X, NT // CORES
    gather = SUB * (Z - 1 + (X - 1) * Y + 3 * NT * S) + S - 1
    back = Y * 2 * SUB + SUB * Z * (2 * (Y - 1) + (X - 1) * (Y + 1) + 2) + NT
    return gather + back


def solution(mesh):
    in_specs = (
        P("ep", None),
        P("ep", None),
        P("ep", None),
        P(),
        P("ep", None, "tp"),
        P("ep", None, "tp"),
        P("ep", "tp", None),
        P("tp"),
    )
    out_specs = P("ep", "tp")
    S, NT = mesh.shape["ep"], mesh.shape["tp"]
    X = 2
    on_device = routed
    if S % X == 0 and NT % CORES == 0 and copies_of(S, X, NT) <= MAX_COPIES:
        on_device = functools.partial(fused, S, X, NT)
    return jax.shard_map(
        on_device, mesh=mesh, in_specs=in_specs, out_specs=out_specs, check_vma=False
    )
```

```python
import functools

import jax
import jax.numpy as jnp
from jax import lax
from jax.experimental import pallas as pl
from jax.experimental.pallas import tpu as pltpu
from jax.sharding import PartitionSpec as P

epsilon = 1e-06
CORES = 2
MESH = pl.DeviceIdType.MESH
VMEM_BYTES = 60 * 1024 * 1024
MAX_COPIES = 512
SUB = 2


def fused_kernel(
    S, X, NT,
    tokens, routes, mix, pre_gain, gate_hbm, up_hbm, down_hbm, post_gain, out,
    xg, wg, wu, wd, acc_g, acc_u, hid, wt, wr,
    pown, dsend, drecv, ya, yar, xb, xbr, xa, xar, yb, ybr, keep_a, keep_b,
    za, zar, zb, zbr, st,
    wsem, ssem, gsem, mixr, dsem, yarsem, xbrsem, xarsem, ybrsem, zarsem, zbrsem, stsem,
):
    R = tokens.shape[0]
    Z, Y = S // X, NT // CORES
    Dq = xg.shape[2]
    W = 2 * SUB
    H = Dq // W
    D = tokens.shape[1]
    K = routes.shape[0]
    R2 = R // SUB
    me, t = lax.axis_index("ep"), lax.axis_index("tp")
    z, x = me // X, lax.rem(me, X)
    y, c = t // CORES, lax.rem(t, CORES)
    pc = 1 - c
    f32, bf16 = jnp.float32, jnp.bfloat16

    def dev(e, q):
        return (e, q)

    def quarter(yy, cc):
        return yy * CORES + cc

    def flip(v, m):
        for b in range(m.bit_length()):
            if m >> b & 1:
                v = v + (1 << b) * (1 - 2 * lax.rem(v // (1 << b), 2))
        return v

    if Z & (Z - 1) == 0:
        zs = [z] + [flip(z, m) for m in range(Z - 1, 0, -1)]
        zm = zs
        near = Z - 1
    else:
        near = 0
        zs = [lax.rem(z + d, Z) for d in range(Z)]
        zm = [lax.rem(z - d + Z, Z) for d in range(Z)]
    xs = [lax.rem(x + d, X) for d in range(X)]
    ys = [lax.rem(y + d, Y) for d in range(Y)]
    xm = [lax.rem(x - d + X, X) for d in range(X)]
    ym = [lax.rem(y - d + Y, Y) for d in range(Y)]

    loads = []
    for i in range(NT):
        for k, (src, dst) in enumerate(((gate_hbm, wg), (up_hbm, wu))):
            loads.append(pltpu.make_async_copy(src.at[0, pl.ds(i * Dq, Dq)], dst.at[i], wsem.at[k, i]))
    for i in range(NT):
        loads.append(pltpu.make_async_copy(down_hbm.at[0, :, pl.ds(i * Dq, Dq)], wd.at[i], wsem.at[2, i]))
    for copy in loads:
        copy.start()

    barrier = pltpu.get_barrier_semaphore()
    for d in range(1, S):
        pl.semaphore_signal(barrier, inc=1, device_id=dev(lax.rem(me + d, S), t), device_id_type=MESH)
    for d in range(1, NT):
        pl.semaphore_signal(barrier, inc=1, device_id=dev(me, lax.rem(t + d, NT)), device_id_type=MESH)

    floats = tokens[...].astype(f32)
    inv = lax.rsqrt(jnp.mean(floats * floats, axis=1, keepdims=True) + epsilon)
    rows = pl.ds(pl.multiple_of(me * R, R), R)
    for q in range(NT):
        cols = slice(q * Dq, (q + 1) * Dq)
        xg[q, rows, :] = (floats[:, cols] * inv * pre_gain[:, cols]).astype(bf16)

    for e in range(S):
        dense = jnp.zeros((1, R), f32)
        for k in range(K):
            dense = dense + jnp.where(routes[k : k + 1, :] == e, mix[k : k + 1, :], 0.0)
        wt[e] = jnp.concatenate([dense, jnp.zeros((1, 128 - R), f32)], axis=1)
    wr[me] = wt[me]

    pl.semaphore_wait(barrier, S - 1 + NT - 1)

    sends = []

    def send(src, dst, recv_sem, device):
        copy = pltpu.make_async_remote_copy(
            src_ref=src, dst_ref=dst, send_sem=ssem.at[len(sends)], recv_sem=recv_sem,
            device_id=device, device_id_type=MESH,
        )
        copy.start()
        sends.append(copy)

    def arrived(ref, sem):
        pltpu.make_async_remote_copy(
            src_ref=ref, dst_ref=ref, send_sem=ssem.at[0], recv_sem=sem,
            device_id=dev(me, t), device_id_type=MESH,
        ).wait_recv()

    def block(q, s, i):
        return xg.at[q, pl.ds(pl.multiple_of(s * R + i * R2, R2), R2)]

    def send_block(q, s, i, device):
        send(block(q, s, i), block(q, s, i), gsem.at[q, s, i], device)

    def await_block(q, s):
        for i in range(SUB):
            arrived(block(q, s, i), gsem.at[q, s, i])

    def await_part(q, s, i):
        arrived(block(q, s, i), gsem.at[q, s, i])

    def at(d, dx):
        return zm[d] * X + xm[dx]

    for d in range(1, Z):
        for i in range(SUB):
            send_block(t, me, i, dev(zs[d] * X + x, t))
            if d == near:
                for dy in range(1, Y):
                    send_block(quarter(ys[dy], c), me, i, dev(zs[d] * X + x, t))
    for dx in range(1, X):
        for i in range(SUB):
            send_block(t, me, i, dev(z * X + xs[dx], t))
            for dy in range(1, Y):
                send_block(quarter(ys[dy], c), me, i, dev(z * X + xs[dx], t))
    for d in range(1, S):
        e = lax.rem(me + d, S)
        send(wt.at[e], wr.at[me], mixr.at[me], dev(e, t))
    for d in range(1, Z):
        s = at(d, 0)
        for i in range(SUB):
            await_part(t, s, i)
            for dx in range(1, X):
                send_block(t, s, i, dev(z * X + xs[dx], t))
            if d != near:
                for dy in range(1, Y):
                    send_block(t, s, i, dev(me, quarter(ys[dy], c)))
            send_block(t, s, i, dev(me, quarter(y, pc)))
            if d == near:
                for dy in range(1, Y):
                    q = quarter(ys[dy], c)
                    await_part(q, s, i)
                    for dx in range(1, X):
                        send_block(q, s, i, dev(z * X + xs[dx], t))
                    send_block(q, s, i, dev(me, quarter(y, pc)))
    for dx in range(1, X):
        for d in range(Z):
            s = at(d, dx)
            for i in range(SUB):
                await_part(t, s, i)
                if d not in (0, near):
                    for dy in range(1, Y):
                        send_block(t, s, i, dev(me, quarter(ys[dy], c)))
                send_block(t, s, i, dev(me, quarter(y, pc)))
                if d in (0, near):
                    for dy in range(1, Y):
                        await_part(quarter(ys[dy], c), s, i)
                        send_block(quarter(ys[dy], c), s, i, dev(me, quarter(y, pc)))

    others = [at(d, dx) for dx in range(X) for d in range(Z) if d or dx]

    def multiply(q, first):
        pltpu.make_async_copy(gate_hbm.at[0, pl.ds(0, Dq)], wg.at[q], wsem.at[0, q]).wait()
        pltpu.make_async_copy(up_hbm.at[0, pl.ds(0, Dq)], wu.at[q], wsem.at[1, q]).wait()
        for w, acc in ((wg, acc_g), (wu, acc_u)):
            part = jnp.dot(xg[q], w[q], preferred_element_type=f32)
            acc[...] = part if first else acc[...] + part

    multiply(t, True)
    for s in others:
        await_block(quarter(y, pc), s)
    multiply(quarter(y, pc), False)
    for dy in range(1, Y):
        for dx in range(X):
            for d in range(1, Z):
                if d == near:
                    continue
                s = at(d, dx)
                for i in range(SUB):
                    await_part(quarter(ym[dy], c), s, i)
                    send_block(quarter(ym[dy], c), s, i, dev(me, quarter(y, pc)))
        multiply(quarter(ym[dy], c), False)
    for dy in range(1, Y):
        for s in others:
            await_block(quarter(ym[dy], pc), s)
        multiply(quarter(ym[dy], pc), False)

    for d in range(1, S):
        s = lax.rem(me + d, S)
        arrived(wr.at[s], mixr.at[s])
    named = jnp.concatenate([wr[s] for s in range(S)] + [jnp.zeros((128 - S, 128), f32)], axis=0)
    columns = jnp.transpose(named)
    weight = jnp.concatenate([columns[:R, s : s + 1] for s in range(S)], axis=0)
    gate = acc_g[...]
    hid[...] = (gate / (1.0 + jnp.exp(-gate)) * acc_u[...] * weight).astype(bf16)

    def down(q):
        pltpu.make_async_copy(down_hbm.at[0, :, pl.ds(0, Dq)], wd.at[q], wsem.at[2, q]).wait()
        return jnp.dot(hid[...], wd[q], preferred_element_type=f32)

    y_order = [ys[dy] for dy in range(1, Y)] + [y]
    js = [zs[d] for d in range(1, Z)] + [z]
    first, second = list(range(SUB)), list(range(SUB, W))

    def own(yy, h, j, xx):
        return pown[yy, h, j, xx] + drecv[yy, h, j, xx].astype(f32)

    def await_core(yy, h):
        arrived(drecv.at[yy, h], dsem.at[yy, h])

    for dy in list(range(1, Y)) + [0]:
        yy = ys[dy]
        part = down(quarter(yy, pc)).astype(bf16)
        for h in first + second if dy else second + first:
            for s in range(S):
                dsend[yy, h, s // X, s % X] = part[s * R : (s + 1) * R, h * H : (h + 1) * H]
            send(dsend.at[yy, h], drecv.at[yy, h], dsem.at[yy, h], dev(me, quarter(y, pc)))
        part = down(quarter(yy, c))
        for h in range(W):
            for s in range(S):
                pown[yy, h, s // X, s % X] = part[s * R : (s + 1) * R, h * H : (h + 1) * H]
        if dy:
            for h in first:
                await_core(yy, h)
            for j in js:
                for h in first:
                    for xx in range(X):
                        ya[dy, h, j, xx] = own(yy, h, j, xx).astype(bf16)
                    send(ya.at[dy, h, j], yar.at[dy, h, j], yarsem.at[dy, h, j], dev(me, quarter(yy, c)))
        for h in second:
            await_core(yy, h)
        for j in js:
            for h in second:
                for dx in range(1, X):
                    xb[dx, yy, h - SUB, j] = own(yy, h, j, xs[dx]).astype(bf16)
                    send(
                        xb.at[dx, yy, h - SUB, j], xbr.at[dx, yy, h - SUB, j],
                        xbrsem.at[dx, yy, h - SUB, j], dev(z * X + xs[dx], t),
                    )
    for h in first:
        await_core(y, h)
    for j in js:
        for i in range(SUB):
            for yy in y_order:
                total = own(yy, SUB + i, j, x)
                for dx in range(1, X):
                    arrived(xbr.at[dx, yy, i, j], xbrsem.at[dx, yy, i, j])
                    total = total + xbr[dx, yy, i, j].astype(f32)
                keep_b[yy, i, j] = total
            for dy in range(1, Y):
                yb[dy, i, j] = keep_b[ys[dy], i, j].astype(bf16)
                send(yb.at[dy, i, j], ybr.at[dy, i, j], ybrsem.at[dy, i, j], dev(me, quarter(ys[dy], c)))
            for dy in range(1, Y):
                arrived(yar.at[dy, i, j], yarsem.at[dy, i, j])
            for dx in list(range(1, X)) + [0]:
                total = own(y, i, j, xs[dx])
                for dy in range(1, Y):
                    total = total + yar[dy, i, j, xs[dx]].astype(f32)
                if dx == 0:
                    keep_a[i, j] = total
                else:
                    xa[dx, i, j] = total.astype(bf16)
                    send(xa.at[dx, i, j], xar.at[dx, i, j], xarsem.at[dx, i, j], dev(z * X + xs[dx], t))
    mine = {}
    for at_d, j in enumerate(js):
        d = (at_d + 1) % Z
        for i in range(SUB):
            total = keep_a[i, j]
            for dx in range(1, X):
                arrived(xar.at[dx, i, j], xarsem.at[dx, i, j])
                total = total + xar[dx, i, j].astype(f32)
            if d:
                za[d, i] = total.astype(bf16)
                send(za.at[d, i], zar.at[d, i], zarsem.at[d, i], dev(j * X + x, t))
            else:
                mine[i] = total
            total = keep_b[y, i, j]
            for dy in range(1, Y):
                arrived(ybr.at[dy, i, j], ybrsem.at[dy, i, j])
                total = total + ybr[dy, i, j].astype(f32)
            if d:
                zb[d, i] = total.astype(bf16)
                send(zb.at[d, i], zbr.at[d, i], zbrsem.at[d, i], dev(j * X + x, t))
            else:
                mine[SUB + i] = total
    for d in range(1, Z):
        for i in range(SUB):
            arrived(zar.at[d, i], zarsem.at[d, i])
            mine[i] = mine[i] + zar[d, i].astype(f32)
            arrived(zbr.at[d, i], zbrsem.at[d, i])
            mine[SUB + i] = mine[SUB + i] + zbr[d, i].astype(f32)

    squares = jnp.zeros((R, 1), f32)
    for h in range(W):
        squares = squares + jnp.sum(mine[h] * mine[h], axis=1, keepdims=True)
    st[0] = jnp.broadcast_to(squares, (R, 128))
    for d in range(1, NT):
        send(st.at[0], st.at[d], stsem.at[d], dev(me, lax.rem(t + d, NT)))
    for d in range(1, NT):
        arrived(st.at[d], stsem.at[d])
        squares = squares + st[d][:, 0:1]
    scale = lax.rsqrt(squares / D + epsilon)
    for h in range(W):
        cols = slice(h * H, (h + 1) * H)
        out[:, cols] = (mine[h] * scale * post_gain[:, cols]).astype(bf16)
    for copy in sends:
        copy.wait_send()


def fused(S, X, NT, tokens, routes, mix_weights, pre_gain, gate_weight, up_weight, down_weight, post_gain):
    R, D = tokens.shape
    F = gate_weight.shape[2]
    Dq = D // NT
    W = 2 * SUB
    H = Dq // W
    Z, Y = S // X, NT // CORES
    f32, bf16 = jnp.float32, jnp.bfloat16
    dma, vmem = pltpu.SemaphoreType.DMA, pltpu.VMEM
    in_vmem, anywhere = pl.BlockSpec(memory_space=pltpu.VMEM), pl.BlockSpec(memory_space=pl.ANY)
    return pl.pallas_call(
        functools.partial(fused_kernel, S, X, NT),
        out_shape=jax.ShapeDtypeStruct((R, Dq), bf16),
        in_specs=[in_vmem] * 4 + [anywhere] * 3 + [in_vmem],
        out_specs=in_vmem,
        scratch_shapes=[
            vmem((NT, S * R, Dq), bf16),
            vmem((NT, Dq, F), bf16),
            vmem((NT, Dq, F), bf16),
            vmem((NT, F, Dq), bf16),
            vmem((S * R, F), f32),
            vmem((S * R, F), f32),
            vmem((S * R, F), bf16),
            vmem((S, 1, 128), f32),
            vmem((S, 1, 128), f32),
            vmem((Y, W, Z, X, R, H), f32),
            vmem((Y, W, Z, X, R, H), bf16),
            vmem((Y, W, Z, X, R, H), bf16),
            vmem((Y, SUB, Z, X, R, H), bf16),
            vmem((Y, SUB, Z, X, R, H), bf16),
            vmem((X, Y, SUB, Z, R, H), bf16),
            vmem((X, Y, SUB, Z, R, H), bf16),
            vmem((X, SUB, Z, R, H), bf16),
            vmem((X, SUB, Z, R, H), bf16),
            vmem((Y, SUB, Z, R, H), bf16),
            vmem((Y, SUB, Z, R, H), bf16),
            vmem((SUB, Z, R, H), f32),
            vmem((Y, SUB, Z, R, H), f32),
            vmem((Z, SUB, R, H), bf16),
            vmem((Z, SUB, R, H), bf16),
            vmem((Z, SUB, R, H), bf16),
            vmem((Z, SUB, R, H), bf16),
            vmem((NT, R, 128), f32),
            dma((3, NT)),
            dma((copies_of(S, X, NT),)),
            dma((NT, S, SUB)),
            dma((S,)),
            dma((Y, W)),
            dma((Y, SUB, Z)),
            dma((X, Y, SUB, Z)),
            dma((X, SUB, Z)),
            dma((Y, SUB, Z)),
            dma((Z, SUB)),
            dma((Z, SUB)),
            dma((NT,)),
        ],
        compiler_params=pltpu.CompilerParams(
            collective_id=0, has_side_effects=True, vmem_limit_bytes=VMEM_BYTES
        ),
    )(
        tokens, routes.T, mix_weights.T, pre_gain.reshape(1, D), gate_weight, up_weight, down_weight,
        post_gain.reshape(1, Dq),
    )


def routed(
    tokens, routes, mix_weights, pre_gain, gate_weight, up_weight, down_weight, post_gain
):
    tok_rows, width = tokens.shape
    top_count = routes.shape[1]
    experts = lax.axis_size("ep")
    capacity = min(tok_rows, max(2, (3 * tok_rows * top_count + 2 * experts - 1) // (2 * experts)))
    floats = tokens.astype(jnp.float32)
    normed = (
        floats * lax.rsqrt(jnp.mean(floats * floats, axis=-1, keepdims=True) + epsilon) * pre_gain
    ).astype(jnp.bfloat16)
    chosen = routes.reshape(-1)
    onehot = (chosen[:, None] == jnp.arange(experts, dtype=jnp.int32)[None, :]).astype(jnp.int32)
    before = jnp.cumsum(onehot, axis=0) - onehot
    slot_rank = jnp.sum(before * onehot, axis=1)
    target = chosen * capacity + slot_rank
    placed = target[:, None] == jnp.arange(experts * capacity, dtype=jnp.int32)[None, :]
    by_choice = placed.reshape(tok_rows, top_count, experts * capacity)
    picked = jnp.any(by_choice, axis=1).astype(jnp.bfloat16)
    outgoing = jnp.einsum("tc,td->cd", picked, normed, preferred_element_type=jnp.float32).astype(
        jnp.bfloat16
    )
    outgoing = outgoing.reshape(experts, capacity, width)
    slice_width = width // lax.axis_size("tp")
    outgoing_part = lax.dynamic_slice_in_dim(
        outgoing, lax.axis_index("tp") * slice_width, slice_width, 2
    )
    arrived = lax.all_to_all(outgoing_part, "ep", split_axis=0, concat_axis=0, tiled=True)
    arrived = lax.all_gather(arrived, "tp", axis=2, tiled=True)
    arrived_rows = arrived.reshape(experts * capacity, width)
    gate_act = jnp.dot(arrived_rows, gate_weight[0], preferred_element_type=jnp.float32)
    up_act = jnp.dot(arrived_rows, up_weight[0], preferred_element_type=jnp.float32)
    hidden = (jax.nn.silu(gate_act) * up_act).astype(jnp.bfloat16)
    partial_value = jnp.dot(hidden, down_weight[0], preferred_element_type=jnp.float32)
    summed = lax.psum_scatter(
        partial_value.astype(jnp.bfloat16), "tp", scatter_dimension=1, tiled=True
    )
    returned = lax.all_to_all(
        summed.reshape(experts, capacity, summed.shape[1]),
        "ep",
        split_axis=0,
        concat_axis=0,
        tiled=True,
    )
    results = returned.reshape(experts * capacity, summed.shape[1]).astype(jnp.float32)
    mixing = jnp.sum(mix_weights[:, :, None] * by_choice.astype(jnp.float32), axis=1)
    mixed = jnp.dot(mixing, results, precision=lax.Precision.HIGHEST)
    squares = jnp.sum(mixed * mixed, axis=1)
    total = lax.psum(squares, "tp")
    scale = lax.rsqrt(total / width + epsilon)
    return (mixed * scale[:, None] * post_gain).astype(jnp.bfloat16)


def copies_of(S, X, NT):
    Z, Y = S // X, NT // CORES
    gather = SUB * ((Z - 1 + X - 1) * Y + 3 * NT * S) + S - 1
    back = Y * 2 * SUB + SUB * Z * (2 * (Y - 1) + (X - 1) * (Y + 1) + 2) + NT
    return gather + back


def solution(mesh):
    in_specs = (
        P("ep", None),
        P("ep", None),
        P("ep", None),
        P(),
        P("ep", None, "tp"),
        P("ep", None, "tp"),
        P("ep", "tp", None),
        P("tp"),
    )
    out_specs = P("ep", "tp")
    S, NT = mesh.shape["ep"], mesh.shape["tp"]
    X = 2
    on_device = routed
    if S % X == 0 and NT % CORES == 0 and copies_of(S, X, NT) <= MAX_COPIES:
        on_device = functools.partial(fused, S, X, NT)
    return jax.shard_map(
        on_device, mesh=mesh, in_specs=in_specs, out_specs=out_specs, check_vma=False
    )
```

```python
import functools

import jax
import jax.numpy as jnp
from jax import lax
from jax.experimental import pallas as pl
from jax.experimental.pallas import tpu as pltpu
from jax.sharding import PartitionSpec as P

epsilon = 1e-06
CORES = 2
MESH = pl.DeviceIdType.MESH
VMEM_BYTES = 60 * 1024 * 1024
MAX_COPIES = 512
SUB = 1


def fused_kernel(
    S, X, NT,
    tokens, routes, mix, pre_gain, gate_hbm, up_hbm, down_hbm, post_gain, out,
    xg, wg, wu, wd, acc_g, acc_u, hid, wt, wr,
    pown, dsend, drecv, ya, yar, xb, xbr, xa, xar, yb, ybr, keep_a, keep_b,
    za, zar, zb, zbr, st,
    wsem, ssem, gsem, mixr, dsem, yarsem, xbrsem, xarsem, ybrsem, zarsem, zbrsem, stsem,
):
    R = tokens.shape[0]
    Z, Y = S // X, NT // CORES
    Dq = xg.shape[2]
    W = 2 * SUB
    H = Dq // W
    D = tokens.shape[1]
    K = routes.shape[0]
    R2 = R // SUB
    me, t = lax.axis_index("ep"), lax.axis_index("tp")
    z, x = me // X, lax.rem(me, X)
    y, c = t // CORES, lax.rem(t, CORES)
    pc = 1 - c
    f32, bf16 = jnp.float32, jnp.bfloat16

    def dev(e, q):
        return (e, q)

    def quarter(yy, cc):
        return yy * CORES + cc

    def flip(v, m):
        for b in range(m.bit_length()):
            if m >> b & 1:
                v = v + (1 << b) * (1 - 2 * lax.rem(v // (1 << b), 2))
        return v

    if Z & (Z - 1) == 0:
        zs = [z] + [flip(z, m) for m in range(1, Z)]
        zm = zs
        near = 1
    else:
        near = 0
        zs = [lax.rem(z + d, Z) for d in range(Z)]
        zm = [lax.rem(z - d + Z, Z) for d in range(Z)]
    xs = [lax.rem(x + d, X) for d in range(X)]
    ys = [lax.rem(y + d, Y) for d in range(Y)]
    xm = [lax.rem(x - d + X, X) for d in range(X)]
    ym = [lax.rem(y - d + Y, Y) for d in range(Y)]

    loads = []
    for i in range(NT):
        for k, (src, dst) in enumerate(((gate_hbm, wg), (up_hbm, wu))):
            loads.append(pltpu.make_async_copy(src.at[0, pl.ds(i * Dq, Dq)], dst.at[i], wsem.at[k, i]))
    for i in range(NT):
        loads.append(pltpu.make_async_copy(down_hbm.at[0, :, pl.ds(i * Dq, Dq)], wd.at[i], wsem.at[2, i]))
    for copy in loads:
        copy.start()

    barrier = pltpu.get_barrier_semaphore()
    for d in range(1, S):
        pl.semaphore_signal(barrier, inc=1, device_id=dev(lax.rem(me + d, S), t), device_id_type=MESH)
    for d in range(1, NT):
        pl.semaphore_signal(barrier, inc=1, device_id=dev(me, lax.rem(t + d, NT)), device_id_type=MESH)

    floats = tokens[...].astype(f32)
    inv = lax.rsqrt(jnp.mean(floats * floats, axis=1, keepdims=True) + epsilon)
    rows = pl.ds(pl.multiple_of(me * R, R), R)
    for q in range(NT):
        cols = slice(q * Dq, (q + 1) * Dq)
        xg[q, rows, :] = (floats[:, cols] * inv * pre_gain[:, cols]).astype(bf16)

    for e in range(S):
        dense = jnp.zeros((1, R), f32)
        for k in range(K):
            dense = dense + jnp.where(routes[k : k + 1, :] == e, mix[k : k + 1, :], 0.0)
        wt[e] = jnp.concatenate([dense, jnp.zeros((1, 128 - R), f32)], axis=1)
    wr[me] = wt[me]

    pl.semaphore_wait(barrier, S - 1 + NT - 1)

    sends = []

    def send(src, dst, recv_sem, device):
        copy = pltpu.make_async_remote_copy(
            src_ref=src, dst_ref=dst, send_sem=ssem.at[len(sends)], recv_sem=recv_sem,
            device_id=device, device_id_type=MESH,
        )
        copy.start()
        sends.append(copy)

    def arrived(ref, sem):
        pltpu.make_async_remote_copy(
            src_ref=ref, dst_ref=ref, send_sem=ssem.at[0], recv_sem=sem,
            device_id=dev(me, t), device_id_type=MESH,
        ).wait_recv()

    def block(q, s, i):
        return xg.at[q, pl.ds(pl.multiple_of(s * R + i * R2, R2), R2)]

    def send_block(q, s, i, device):
        send(block(q, s, i), block(q, s, i), gsem.at[q, s, i], device)

    def await_block(q, s):
        for i in range(SUB):
            arrived(block(q, s, i), gsem.at[q, s, i])

    def await_part(q, s, i):
        arrived(block(q, s, i), gsem.at[q, s, i])

    def at(d, dx):
        return zm[d] * X + xm[dx]

    for d in range(1, Z):
        for i in range(SUB):
            send_block(t, me, i, dev(zs[d] * X + x, t))
            if d == near:
                for dy in range(1, Y):
                    send_block(quarter(ys[dy], c), me, i, dev(zs[d] * X + x, t))
    for dx in range(1, X):
        for i in range(SUB):
            send_block(t, me, i, dev(z * X + xs[dx], t))
            for dy in range(1, Y):
                send_block(quarter(ys[dy], c), me, i, dev(z * X + xs[dx], t))
    for d in range(1, S):
        e = lax.rem(me + d, S)
        send(wt.at[e], wr.at[me], mixr.at[me], dev(e, t))
    for d in range(1, Z):
        s = at(d, 0)
        for i in range(SUB):
            await_part(t, s, i)
            for dx in range(1, X):
                send_block(t, s, i, dev(z * X + xs[dx], t))
            if d != near:
                for dy in range(1, Y):
                    send_block(t, s, i, dev(me, quarter(ys[dy], c)))
            send_block(t, s, i, dev(me, quarter(y, pc)))
            if d == near:
                for dy in range(1, Y):
                    q = quarter(ys[dy], c)
                    await_part(q, s, i)
                    for dx in range(1, X):
                        send_block(q, s, i, dev(z * X + xs[dx], t))
                    send_block(q, s, i, dev(me, quarter(y, pc)))
    for dx in range(1, X):
        for d in range(Z):
            s = at(d, dx)
            for i in range(SUB):
                await_part(t, s, i)
                if d not in (0, near):
                    for dy in range(1, Y):
                        send_block(t, s, i, dev(me, quarter(ys[dy], c)))
                send_block(t, s, i, dev(me, quarter(y, pc)))
                if d in (0, near):
                    for dy in range(1, Y):
                        await_part(quarter(ys[dy], c), s, i)
                        send_block(quarter(ys[dy], c), s, i, dev(me, quarter(y, pc)))

    others = [at(d, dx) for dx in range(X) for d in range(Z) if d or dx]

    def multiply(q, first):
        pltpu.make_async_copy(gate_hbm.at[0, pl.ds(0, Dq)], wg.at[q], wsem.at[0, q]).wait()
        pltpu.make_async_copy(up_hbm.at[0, pl.ds(0, Dq)], wu.at[q], wsem.at[1, q]).wait()
        for w, acc in ((wg, acc_g), (wu, acc_u)):
            part = jnp.dot(xg[q], w[q], preferred_element_type=f32)
            acc[...] = part if first else acc[...] + part

    multiply(t, True)
    for s in others:
        await_block(quarter(y, pc), s)
    multiply(quarter(y, pc), False)
    for dy in range(1, Y):
        for dx in range(X):
            for d in range(1, Z):
                if d == near:
                    continue
                s = at(d, dx)
                for i in range(SUB):
                    await_part(quarter(ym[dy], c), s, i)
                    send_block(quarter(ym[dy], c), s, i, dev(me, quarter(y, pc)))
        multiply(quarter(ym[dy], c), False)
    for dy in range(1, Y):
        for s in others:
            await_block(quarter(ym[dy], pc), s)
        multiply(quarter(ym[dy], pc), False)

    for d in range(1, S):
        s = lax.rem(me + d, S)
        arrived(wr.at[s], mixr.at[s])
    named = jnp.concatenate([wr[s] for s in range(S)] + [jnp.zeros((128 - S, 128), f32)], axis=0)
    columns = jnp.transpose(named)
    weight = jnp.concatenate([columns[:R, s : s + 1] for s in range(S)], axis=0)
    gate = acc_g[...]
    hid[...] = (gate / (1.0 + jnp.exp(-gate)) * acc_u[...] * weight).astype(bf16)

    def down(q):
        pltpu.make_async_copy(down_hbm.at[0, :, pl.ds(0, Dq)], wd.at[q], wsem.at[2, q]).wait()
        return jnp.dot(hid[...], wd[q], preferred_element_type=f32)

    y_order = [ys[dy] for dy in range(1, Y)] + [y]
    js = [zs[d] for d in range(1, Z)] + [z]
    first, second = list(range(SUB)), list(range(SUB, W))

    def own(yy, h, j, xx):
        return pown[yy, h, j, xx] + drecv[yy, h, j, xx].astype(f32)

    def await_core(yy, h):
        arrived(drecv.at[yy, h], dsem.at[yy, h])

    for dy in list(range(1, Y)) + [0]:
        yy = ys[dy]
        part = down(quarter(yy, pc)).astype(bf16)
        for h in first + second if dy else second + first:
            for s in range(S):
                dsend[yy, h, s // X, s % X] = part[s * R : (s + 1) * R, h * H : (h + 1) * H]
            send(dsend.at[yy, h], drecv.at[yy, h], dsem.at[yy, h], dev(me, quarter(y, pc)))
        part = down(quarter(yy, c))
        for h in range(W):
            for s in range(S):
                pown[yy, h, s // X, s % X] = part[s * R : (s + 1) * R, h * H : (h + 1) * H]
        if dy:
            for h in first:
                await_core(yy, h)
            for j in js:
                for h in first:
                    for xx in range(X):
                        ya[dy, h, j, xx] = own(yy, h, j, xx).astype(bf16)
                    send(ya.at[dy, h, j], yar.at[dy, h, j], yarsem.at[dy, h, j], dev(me, quarter(yy, c)))
        for h in second:
            await_core(yy, h)
        for j in js:
            for h in second:
                for dx in range(1, X):
                    xb[dx, yy, h - SUB, j] = own(yy, h, j, xs[dx]).astype(bf16)
                    send(
                        xb.at[dx, yy, h - SUB, j], xbr.at[dx, yy, h - SUB, j],
                        xbrsem.at[dx, yy, h - SUB, j], dev(z * X + xs[dx], t),
                    )
    for h in first:
        await_core(y, h)
    for j in js:
        for i in range(SUB):
            for yy in y_order:
                total = own(yy, SUB + i, j, x)
                for dx in range(1, X):
                    arrived(xbr.at[dx, yy, i, j], xbrsem.at[dx, yy, i, j])
                    total = total + xbr[dx, yy, i, j].astype(f32)
                keep_b[yy, i, j] = total
            for dy in range(1, Y):
                yb[dy, i, j] = keep_b[ys[dy], i, j].astype(bf16)
                send(yb.at[dy, i, j], ybr.at[dy, i, j], ybrsem.at[dy, i, j], dev(me, quarter(ys[dy], c)))
            for dy in range(1, Y):
                arrived(yar.at[dy, i, j], yarsem.at[dy, i, j])
            for dx in list(range(1, X)) + [0]:
                total = own(y, i, j, xs[dx])
                for dy in range(1, Y):
                    total = total + yar[dy, i, j, xs[dx]].astype(f32)
                if dx == 0:
                    keep_a[i, j] = total
                else:
                    xa[dx, i, j] = total.astype(bf16)
                    send(xa.at[dx, i, j], xar.at[dx, i, j], xarsem.at[dx, i, j], dev(z * X + xs[dx], t))
    mine = {}
    for at_d, j in enumerate(js):
        d = (at_d + 1) % Z
        for i in range(SUB):
            total = keep_a[i, j]
            for dx in range(1, X):
                arrived(xar.at[dx, i, j], xarsem.at[dx, i, j])
                total = total + xar[dx, i, j].astype(f32)
            if d:
                za[d, i] = total.astype(bf16)
                send(za.at[d, i], zar.at[d, i], zarsem.at[d, i], dev(j * X + x, t))
            else:
                mine[i] = total
            total = keep_b[y, i, j]
            for dy in range(1, Y):
                arrived(ybr.at[dy, i, j], ybrsem.at[dy, i, j])
                total = total + ybr[dy, i, j].astype(f32)
            if d:
                zb[d, i] = total.astype(bf16)
                send(zb.at[d, i], zbr.at[d, i], zbrsem.at[d, i], dev(j * X + x, t))
            else:
                mine[SUB + i] = total
    for d in range(1, Z):
        for i in range(SUB):
            arrived(zar.at[d, i], zarsem.at[d, i])
            mine[i] = mine[i] + zar[d, i].astype(f32)
            arrived(zbr.at[d, i], zbrsem.at[d, i])
            mine[SUB + i] = mine[SUB + i] + zbr[d, i].astype(f32)

    squares = jnp.zeros((R, 1), f32)
    for h in range(W):
        squares = squares + jnp.sum(mine[h] * mine[h], axis=1, keepdims=True)
    st[0] = jnp.broadcast_to(squares, (R, 128))
    for d in range(1, NT):
        send(st.at[0], st.at[d], stsem.at[d], dev(me, lax.rem(t + d, NT)))
    for d in range(1, NT):
        arrived(st.at[d], stsem.at[d])
        squares = squares + st[d][:, 0:1]
    scale = lax.rsqrt(squares / D + epsilon)
    for h in range(W):
        cols = slice(h * H, (h + 1) * H)
        out[:, cols] = (mine[h] * scale * post_gain[:, cols]).astype(bf16)
    for copy in sends:
        copy.wait_send()


def fused(S, X, NT, tokens, routes, mix_weights, pre_gain, gate_weight, up_weight, down_weight, post_gain):
    R, D = tokens.shape
    F = gate_weight.shape[2]
    Dq = D // NT
    W = 2 * SUB
    H = Dq // W
    Z, Y = S // X, NT // CORES
    f32, bf16 = jnp.float32, jnp.bfloat16
    dma, vmem = pltpu.SemaphoreType.DMA, pltpu.VMEM
    in_vmem, anywhere = pl.BlockSpec(memory_space=pltpu.VMEM), pl.BlockSpec(memory_space=pl.ANY)
    return pl.pallas_call(
        functools.partial(fused_kernel, S, X, NT),
        out_shape=jax.ShapeDtypeStruct((R, Dq), bf16),
        in_specs=[in_vmem] * 4 + [anywhere] * 3 + [in_vmem],
        out_specs=in_vmem,
        scratch_shapes=[
            vmem((NT, S * R, Dq), bf16),
            vmem((NT, Dq, F), bf16),
            vmem((NT, Dq, F), bf16),
            vmem((NT, F, Dq), bf16),
            vmem((S * R, F), f32),
            vmem((S * R, F), f32),
            vmem((S * R, F), bf16),
            vmem((S, 1, 128), f32),
            vmem((S, 1, 128), f32),
            vmem((Y, W, Z, X, R, H), f32),
            vmem((Y, W, Z, X, R, H), bf16),
            vmem((Y, W, Z, X, R, H), bf16),
            vmem((Y, SUB, Z, X, R, H), bf16),
            vmem((Y, SUB, Z, X, R, H), bf16),
            vmem((X, Y, SUB, Z, R, H), bf16),
            vmem((X, Y, SUB, Z, R, H), bf16),
            vmem((X, SUB, Z, R, H), bf16),
            vmem((X, SUB, Z, R, H), bf16),
            vmem((Y, SUB, Z, R, H), bf16),
            vmem((Y, SUB, Z, R, H), bf16),
            vmem((SUB, Z, R, H), f32),
            vmem((Y, SUB, Z, R, H), f32),
            vmem((Z, SUB, R, H), bf16),
            vmem((Z, SUB, R, H), bf16),
            vmem((Z, SUB, R, H), bf16),
            vmem((Z, SUB, R, H), bf16),
            vmem((NT, R, 128), f32),
            dma((3, NT)),
            dma((copies_of(S, X, NT),)),
            dma((NT, S, SUB)),
            dma((S,)),
            dma((Y, W)),
            dma((Y, SUB, Z)),
            dma((X, Y, SUB, Z)),
            dma((X, SUB, Z)),
            dma((Y, SUB, Z)),
            dma((Z, SUB)),
            dma((Z, SUB)),
            dma((NT,)),
        ],
        compiler_params=pltpu.CompilerParams(
            collective_id=0, has_side_effects=True, vmem_limit_bytes=VMEM_BYTES
        ),
    )(
        tokens, routes.T, mix_weights.T, pre_gain.reshape(1, D), gate_weight, up_weight, down_weight,
        post_gain.reshape(1, Dq),
    )


def routed(
    tokens, routes, mix_weights, pre_gain, gate_weight, up_weight, down_weight, post_gain
):
    tok_rows, width = tokens.shape
    top_count = routes.shape[1]
    experts = lax.axis_size("ep")
    capacity = min(tok_rows, max(2, (3 * tok_rows * top_count + 2 * experts - 1) // (2 * experts)))
    floats = tokens.astype(jnp.float32)
    normed = (
        floats * lax.rsqrt(jnp.mean(floats * floats, axis=-1, keepdims=True) + epsilon) * pre_gain
    ).astype(jnp.bfloat16)
    chosen = routes.reshape(-1)
    onehot = (chosen[:, None] == jnp.arange(experts, dtype=jnp.int32)[None, :]).astype(jnp.int32)
    before = jnp.cumsum(onehot, axis=0) - onehot
    slot_rank = jnp.sum(before * onehot, axis=1)
    target = chosen * capacity + slot_rank
    placed = target[:, None] == jnp.arange(experts * capacity, dtype=jnp.int32)[None, :]
    by_choice = placed.reshape(tok_rows, top_count, experts * capacity)
    picked = jnp.any(by_choice, axis=1).astype(jnp.bfloat16)
    outgoing = jnp.einsum("tc,td->cd", picked, normed, preferred_element_type=jnp.float32).astype(
        jnp.bfloat16
    )
    outgoing = outgoing.reshape(experts, capacity, width)
    slice_width = width // lax.axis_size("tp")
    outgoing_part = lax.dynamic_slice_in_dim(
        outgoing, lax.axis_index("tp") * slice_width, slice_width, 2
    )
    arrived = lax.all_to_all(outgoing_part, "ep", split_axis=0, concat_axis=0, tiled=True)
    arrived = lax.all_gather(arrived, "tp", axis=2, tiled=True)
    arrived_rows = arrived.reshape(experts * capacity, width)
    gate_act = jnp.dot(arrived_rows, gate_weight[0], preferred_element_type=jnp.float32)
    up_act = jnp.dot(arrived_rows, up_weight[0], preferred_element_type=jnp.float32)
    hidden = (jax.nn.silu(gate_act) * up_act).astype(jnp.bfloat16)
    partial_value = jnp.dot(hidden, down_weight[0], preferred_element_type=jnp.float32)
    summed = lax.psum_scatter(
        partial_value.astype(jnp.bfloat16), "tp", scatter_dimension=1, tiled=True
    )
    returned = lax.all_to_all(
        summed.reshape(experts, capacity, summed.shape[1]),
        "ep",
        split_axis=0,
        concat_axis=0,
        tiled=True,
    )
    results = returned.reshape(experts * capacity, summed.shape[1]).astype(jnp.float32)
    mixing = jnp.sum(mix_weights[:, :, None] * by_choice.astype(jnp.float32), axis=1)
    mixed = jnp.dot(mixing, results, precision=lax.Precision.HIGHEST)
    squares = jnp.sum(mixed * mixed, axis=1)
    total = lax.psum(squares, "tp")
    scale = lax.rsqrt(total / width + epsilon)
    return (mixed * scale[:, None] * post_gain).astype(jnp.bfloat16)


def copies_of(S, X, NT):
    Z, Y = S // X, NT // CORES
    gather = SUB * ((Z - 1 + X - 1) * Y + 3 * NT * S) + S - 1
    back = Y * 2 * SUB + SUB * Z * (2 * (Y - 1) + (X - 1) * (Y + 1) + 2) + NT
    return gather + back


def solution(mesh):
    in_specs = (
        P("ep", None),
        P("ep", None),
        P("ep", None),
        P(),
        P("ep", None, "tp"),
        P("ep", None, "tp"),
        P("ep", "tp", None),
        P("tp"),
    )
    out_specs = P("ep", "tp")
    S, NT = mesh.shape["ep"], mesh.shape["tp"]
    X = 2
    on_device = routed
    if S % X == 0 and NT % CORES == 0 and copies_of(S, X, NT) <= MAX_COPIES:
        on_device = functools.partial(fused, S, X, NT)
    return jax.shard_map(
        on_device, mesh=mesh, in_specs=in_specs, out_specs=out_specs, check_vma=False
    )
```
